32 devices in a mesh: sp: 4 (over y, core), dp: 8 (over z, x).
Axes of the slice: x: 2, y: 2, z: 4, core: 2. Of those that a mesh axis runs over, the one named last changes fastest.
Arguments:
- queries: bfloat16 [8, 704, 2048], P('dp', 'sp'), may hold values from -24 to 24, as said below
- keys: bfloat16 [8, 704, 256], P('dp', 'sp'), may hold values from -24 to 24, as said below
- tokens: bfloat16 [8, 704, 2304], P('dp', 'sp'), may hold values from -18 to 18
- w_value: bfloat16 [2304, 256], P('dp'), may hold values from -0.125 to 0.125
- q_gain: float32 [128], replicated, may hold values from 0.5 to 6, as said below
- k_gain: float32 [128], replicated, may hold values from 0.5 to 6, as said below
Outputs:
- attended: bfloat16 [8, 704, 2048], P('dp', 'sp')
The draws below stay inside these ranges and needn't reach their ends.
Inputs may be any that keep to these rules, and one draw needn't show every extreme that they name: `queries`: real-valued projected query entries. `keys`: real-valued projected key entries. `q_gain`: positive gains. `k_gain`: positive gains.
All inputs are finite; a program needn't handle non-finite values.
Results may differ from the reference program's by a relative error of at most 0.0022.
The reference program's roundings to bfloat16 on the way (of `values`, `query_rot`, `key_rot` and `probability`) count: a program that leaves them out, or rounds other values in their place, can miss the bound.
Values may be sent and summed in bfloat16 or wider, within the bound.
No kernel may reach another device: no remote copies, remote signals or barrier semaphores. Data moves between devices by JAX's collectives and lax.ppermute only.
A program may use at most 64 MiB of HBM per device.

```python
import math
import jax
import jax.numpy as jnp
from jax import lax

D = 2304
HD = 128
QH = 16
KVH = 2
GRID_W = 64
LEN = 704
BATCH = 8


def shared_pair(key):
    key_draw = jnp.clip(jax.random.normal(jax.random.fold_in(key, 11), (BATCH, LEN, KVH * HD), jnp.float32), -6.0, 6.0)
    query_draw = jnp.clip(jax.random.normal(jax.random.fold_in(key, 12), (BATCH, LEN, QH * HD), jnp.float32), -6.0, 6.0)
    return (query_draw, key_draw)


def draw_queries(key, part):
    return shared_pair(key)[0].astype(jnp.bfloat16)


def draw_keys(key, part):
    return shared_pair(key)[1].astype(jnp.bfloat16)


def gain_draw(key):
    return jnp.exp(jax.random.uniform(key, (HD,), jnp.float32, jnp.log(0.6), jnp.log(1.8)))


def draw_q_gain(key, part):
    return gain_draw(jax.random.fold_in(key, 21))


def draw_k_gain(key, part):
    return gain_draw(jax.random.fold_in(key, 22))


def levels(stream_key, dims, shards, smallest, top_value):
    def one(dim, parts):
        heights = jax.random.uniform(jax.random.fold_in(jax.random.fold_in(stream_key, 6), dim), (parts,), jnp.float32, smallest / len(shards), top_value / len(shards))
        return jnp.repeat(jnp.exp(heights), dims[dim] // parts).reshape((-1,) + (1,) * (len(dims) - dim - 1))

    level = one(*shards[0])
    for cut in shards[1:]:
        level = level * one(*cut)
    return level


def normal_values(stream_key, shape, width, most, shards=(), kind=jnp.bfloat16):
    array = jax.random.normal(stream_key, shape, jnp.float32) * width
    if len(shards) > 0:
        array = levels(stream_key, shape, shards, -0.22, 0.18) * array
    return jnp.clip(array, min=-most, max=most).astype(kind)


def setup_inputs(seed: int = 0) -> dict:
    key_list = jax.random.split(jax.random.key(seed), 7)
    queries = draw_queries(jax.random.fold_in(key_list[6], 71), 0)
    keys = draw_keys(jax.random.fold_in(key_list[6], 71), 0)
    tokens = normal_values(key_list[2], (BATCH, LEN, D), 3.0, 18.0, ((0, 8), (1, 4)))
    w_value = normal_values(key_list[3], (D, KVH * HD), D ** -0.5, 0.125, ((0, 8),))
    q_gain = draw_q_gain(jax.random.fold_in(key_list[6], 71), 0)
    k_gain = draw_k_gain(jax.random.fold_in(key_list[6], 71), 0)
    return {"queries": queries, "keys": keys, "tokens": tokens, "w_value": w_value, "q_gain": q_gain, "k_gain": k_gain}


epsilon = 1e-06

def unit_rms(vectors, scaling):
    return vectors * lax.rsqrt(lax.optimization_barrier(jnp.mean(vectors * vectors, axis=-1, keepdims=True)) + epsilon) * scaling

def rotary(vectors, row_pos, col_pos):
    head_width = vectors.shape[-1]
    half_width = head_width // 2
    quarter = half_width // 2
    frequency = 10000.0 ** (-jnp.arange(quarter, dtype=jnp.float32) * 2.0 / half_width)

    def rotate_half(section, angle_pos):
        angles = angle_pos[:, None, None] * frequency
        cosine = jnp.cos(angles)
        sine_table = jnp.sin(angles)
        leading = section[..., :quarter]
        second = section[..., quarter:]
        return jnp.concatenate([leading * cosine - second * sine_table, second * cosine + leading * sine_table], axis=-1)
    return jnp.concatenate([rotate_half(vectors[..., :half_width], row_pos), rotate_half(vectors[..., half_width:], col_pos)], axis=-1)

def reference(queries, keys, tokens, w_value, q_gain, k_gain):
    group = QH // KVH
    positions = jnp.arange(LEN, dtype=jnp.int32)
    row_pos = (positions // GRID_W).astype(jnp.float32)
    col_pos = (positions % GRID_W).astype(jnp.float32)
    block_rows = math.gcd(LEN, 512)

    def one_sequence(inputs):
        query_rows, key_rows, token_rows = inputs
        values = jnp.dot(token_rows, w_value, preferred_element_type=jnp.float32)
        values = lax.optimization_barrier(values.astype(jnp.bfloat16)).astype(jnp.float32).reshape(LEN, KVH, HD)
        query_norm = unit_rms(query_rows.astype(jnp.float32).reshape(LEN, QH, HD), q_gain.astype(jnp.float32))
        query_rot = lax.optimization_barrier(rotary(query_norm, row_pos, col_pos).astype(jnp.bfloat16)).astype(jnp.float32)
        key_norm = unit_rms(key_rows.astype(jnp.float32).reshape(LEN, KVH, HD), k_gain.astype(jnp.float32))
        key_rot = lax.optimization_barrier(rotary(key_norm, row_pos, col_pos).astype(jnp.bfloat16)).astype(jnp.float32)
        blocked = query_rot.reshape(LEN // block_rows, block_rows, KVH, group, HD)

        def one_block(query_block):
            scores = jnp.einsum('qkgd,nkd->kgqn', query_block, key_rot) * HD ** (-0.5)
            highest = lax.optimization_barrier(jnp.max(scores, axis=-1, keepdims=True))
            weights = jnp.exp(scores - highest)
            weights = weights / lax.optimization_barrier(jnp.sum(weights, axis=-1, keepdims=True))
            probability = lax.optimization_barrier(weights.astype(jnp.bfloat16)).astype(jnp.float32)
            blended = jnp.einsum('kgqn,nkd->qkgd', probability, values)
            return blended.astype(jnp.bfloat16).reshape(block_rows, QH * HD)
        return lax.map(one_block, blocked).reshape(LEN, QH * HD)
    return lax.map(one_sequence, (queries, keys, tokens))
```

```python
import functools
import math

import jax
import jax.numpy as jnp
import numpy as np
from jax import lax
from jax.experimental import pallas as pl
from jax.experimental.pallas import tpu as pltpu
from jax.sharding import PartitionSpec as P

HD = 128
QH = 16
KVH = 2
GRID_W = 64
EPS = 1e-06
GROUP = QH // KVH


def rope_tables(length):
    m = HD // 2
    q = m // 2
    freq = (np.float32(10000.0) ** (-np.arange(q, dtype=np.float32) * 2.0 / m)).astype(np.float32)
    t = np.arange(length)
    row = (t // GRID_W).astype(np.float32)[:, None] * freq
    col = (t % GRID_W).astype(np.float32)[:, None] * freq
    ang = np.concatenate([row, row, col, col], axis=1).astype(np.float64)
    second = (np.arange(HD) % m) >= q
    cos = np.cos(ang).astype(np.float32)
    sin = np.sin(ang).astype(np.float32)
    return cos, np.where(second, sin, 0.0).astype(np.float32), np.where(second, 0.0, -sin).astype(np.float32)


def norm_rope(u, gain, cos, s1, s2):
    n = u * lax.rsqrt(jnp.mean(u * u, axis=-1, keepdims=True) + EPS) * gain
    q = HD // 4
    r = n * cos + pltpu.roll(n, q, 1) * s1 + pltpu.roll(n, HD - q, 1) * s2
    return r.astype(jnp.bfloat16)


def prob_kernel(rows, n_sp, idx_ref, q_ref, *refs):
    k_refs = refs[:n_sp]
    qg_ref, kg_ref, cos_ref, s1_ref, s2_ref, p_ref, k_scr = refs[n_sp:]

    def tables(pos):
        start = pl.multiple_of(pos * rows, 16)
        at = pl.ds(start, rows)
        return cos_ref[at, :], s1_ref[at, :], s2_ref[at, :]

    kg = kg_ref[...]
    for j in range(n_sp):
        k_scr[j * rows : (j + 1) * rows, :] = norm_rope(
            k_refs[j][...].astype(jnp.float32), kg, *tables(idx_ref[j])
        )
    qg = qg_ref[...]
    tab = tables(idx_ref[0])
    factor = HD**-0.5 * math.log2(math.e)
    for h in range(GROUP):
        qr = norm_rope(q_ref[:, h * HD : (h + 1) * HD].astype(jnp.float32), qg, *tab)
        s = lax.dot_general(qr, k_scr[...], (((1,), (1,)), ((), ())), preferred_element_type=jnp.float32)
        e = jnp.exp2((s - jnp.max(s, axis=-1, keepdims=True)) * factor)
        r = 1.0 / jnp.sum(e, axis=-1, keepdims=True)
        p_ref[h * rows : (h + 1) * rows, :] = (e * r).astype(jnp.bfloat16)


def probabilities(idx, queries, key_parts, qg, kg, tables, g):
    rows = queries.shape[0]
    n_sp = len(key_parts)
    length = rows * n_sp
    full = lambda a: pl.BlockSpec(a.shape, lambda i: (0, 0))
    return pl.pallas_call(
        functools.partial(prob_kernel, rows, n_sp),
        grid=(1,),
        in_specs=[
            pl.BlockSpec(memory_space=pltpu.SMEM),
            pl.BlockSpec((rows, GROUP * HD), lambda i: (0, g)),
            *[pl.BlockSpec((rows, HD), lambda i: (0, g)) for _ in key_parts],
            full(qg),
            full(kg),
            *[full(t) for t in tables],
        ],
        out_specs=pl.BlockSpec((GROUP * rows, length), lambda i: (0, 0)),
        out_shape=jax.ShapeDtypeStruct((GROUP * rows, length), jnp.bfloat16),
        scratch_shapes=[pltpu.VMEM((length, HD), jnp.bfloat16)],
        name=f"prob{g}",
    )(idx, queries, *key_parts, qg, kg, *tables)


def value_kernel(layout, shard, idx_ref, tok_ref, *refs):
    parts, out_ref, w_scr = refs[:-2], refs[-2], refs[-1]
    half = shard // 2
    for ref, slots in zip(parts, layout):
        for n, (s, side) in enumerate(slots):
            if side is None:
                w_scr[pl.ds(pl.multiple_of(idx_ref[s] * shard, 16), shard), :] = ref[...]
            else:
                start = idx_ref[s] * shard + idx_ref[side] * half
                w_scr[pl.ds(pl.multiple_of(start, 16), half), :] = ref[n * half : (n + 1) * half, :]
    out_ref[...] = jnp.dot(tok_ref[...], w_scr[...], preferred_element_type=jnp.float32).astype(jnp.bfloat16)


def project(idx, tokens, parts, layout, shard):
    rows, width = tokens.shape
    cols = parts[0].shape[1]
    full = lambda a: pl.BlockSpec(a.shape, lambda i: (0, 0))
    return pl.pallas_call(
        functools.partial(value_kernel, layout, shard),
        grid=(1,),
        in_specs=[pl.BlockSpec(memory_space=pltpu.SMEM), full(tokens), *[full(p) for p in parts]],
        out_specs=pl.BlockSpec((rows, cols), lambda i: (0, 0)),
        out_shape=jax.ShapeDtypeStruct((rows, cols), jnp.bfloat16),
        scratch_shapes=[pltpu.VMEM((width, cols), jnp.bfloat16)],
        name="project",
    )(idx, tokens, *parts)


def blend_kernel(rows, n_sp, *refs):
    p_refs = refs[:KVH]
    v_refs = refs[KVH : KVH + n_sp]
    out_ref, v_scr = refs[-2:]
    for j in range(n_sp):
        v_scr[j * rows : (j + 1) * rows, :] = v_refs[j][...]
    for g in range(KVH):
        v = v_scr[:, g * HD : (g + 1) * HD]
        o = jnp.dot(p_refs[g][...], v, preferred_element_type=jnp.float32).astype(jnp.bfloat16)
        for h in range(GROUP):
            at = (g * GROUP + h) * HD
            out_ref[:, at : at + HD] = o[h * rows : (h + 1) * rows, :]


def blend(probs, value_parts):
    rows, cols = value_parts[0].shape
    n_sp = len(value_parts)
    full = lambda a: pl.BlockSpec(a.shape, lambda i: (0, 0))
    return pl.pallas_call(
        functools.partial(blend_kernel, rows, n_sp),
        grid=(1,),
        in_specs=[*[full(p) for p in probs], *[full(v) for v in value_parts]],
        out_specs=pl.BlockSpec((rows, QH * HD), lambda i: (0, 0)),
        out_shape=jax.ShapeDtypeStruct((rows, QH * HD), jnp.bfloat16),
        scratch_shapes=[pltpu.VMEM((rows * n_sp, cols), jnp.bfloat16)],
        name="blend",
    )(*probs, *value_parts)


def swap(x, axis, s):
    return lax.ppermute(x, axis, [(i, i ^ s) for i in range(lax.axis_size(axis))])


def spread(x):
    return [x] + [swap(x, "sp", s) for s in range(1, lax.axis_size("sp"))]


def gather_weights(w):
    n = lax.axis_size("dp")
    shard = w.shape[0]
    if n & (n - 1) or n < 4 or shard % 32:
        return [lax.all_gather(w, "dp", axis=0, tiled=True)], None
    half = shard // 2
    mine, other = n, n + 1
    h = lax.dynamic_slice_in_dim(w, (lax.axis_index("sp") % 2) * half, half, 0)
    z = jnp.concatenate([swap(h, "dp", s) for s in range(2, n, 2)], axis=0)
    x0 = swap(h, "dp", 1)
    xz = swap(z, "dp", 1)
    even = list(range(2, n, 2))
    odd = [s + 1 for s in even]
    parts = [w, z, x0, xz, swap(z, "sp", 1), swap(x0, "sp", 1), swap(xz, "sp", 1)]
    layout = [
        [(0, None)],
        [(s, mine) for s in even],
        [(1, mine)],
        [(s, mine) for s in odd],
        [(s, other) for s in even],
        [(1, other)],
        [(s, other) for s in odd],
    ]
    return parts, layout


def per_device(queries, keys, tokens, w_value, q_gain, k_gain):
    n_sp = lax.axis_size("sp")
    n_dp = lax.axis_size("dp")
    rows = tokens.shape[1]
    me = lax.axis_index("sp").astype(jnp.int32)
    mine = lax.axis_index("dp").astype(jnp.int32)
    parts, layout = gather_weights(w_value)
    shard = w_value.shape[0]
    if layout is None:
        layout, shard = [[(0, None)]], parts[0].shape[0]
        w_idx = jnp.zeros((1,), jnp.int32)
    else:
        w_idx = jnp.concatenate([mine ^ jnp.arange(n_dp, dtype=jnp.int32), jnp.stack([me % 2, 1 - me % 2])])
    sp_idx = me ^ jnp.arange(n_sp, dtype=jnp.int32)
    key_parts = spread(keys[0])
    tables = [jnp.asarray(t) for t in rope_tables(rows * n_sp)]
    qg, kg = q_gain.reshape(1, HD), k_gain.reshape(1, HD)
    probs = [probabilities(sp_idx, queries[0], key_parts, qg, kg, tables, g) for g in range(KVH)]
    values = project(w_idx, tokens[0], parts, layout, shard)
    return blend(probs, spread(values))[None]


def solution(mesh):
    in_specs = (
        P("dp", "sp", None),
        P("dp", "sp", None),
        P("dp", "sp", None),
        P("dp", None),
        P(),
        P(),
    )
    out_specs = P("dp", "sp", None)
    return jax.shard_map(
        per_device, mesh=mesh, in_specs=in_specs, out_specs=out_specs, check_vma=False
    )
```
